32 devices in a mesh: fs: 16 (over z, y, x), tp: 2 (over core).
Axes of the slice: x: 2, y: 2, z: 4, core: 2. Of those that a mesh axis runs over, the one named last changes fastest.
Arguments:
- tokens: bfloat16 [6144, 2048], P('fs', 'tp'), may hold values from -6 to 6
- outer_gate: bfloat16 [2048, 2048], P('fs', 'tp'), may hold values from -0.125 to 0.125
- inner_gate: bfloat16 [2048, 2048], P('fs', 'tp'), may hold values from -0.125 to 0.125
- mix_value: bfloat16 [2048, 2048], P('fs', 'tp'), may hold values from -0.125 to 0.125
- mix_taps: bfloat16 [3, 2048], P(None, 'tp'), may hold values from -3 to 3
- mix_out: bfloat16 [2048, 2048], P('tp', 'fs'), may hold values from -0.1875 to 0.1875
- mix_gain: bfloat16 [2048], P('tp'), may hold values from 0.099609375 to 1.8984375
- ffn_gate: bfloat16 [2048, 3072], P('fs', 'tp'), may hold values from -0.125 to 0.125
- ffn_value: bfloat16 [2048, 3072], P('fs', 'tp'), may hold values from -0.125 to 0.125
- gate_taps: bfloat16 [3, 3072], P(None, 'tp'), may hold values from -3 to 3
- value_taps: bfloat16 [3, 3072], P(None, 'tp'), may hold values from -3 to 3
- ffn_down: bfloat16 [3072, 2048], P('tp', 'fs'), may hold values from -0.15625 to 0.15625
- ffn_gain: bfloat16 [2048], P('tp'), may hold values from 0.099609375 to 1.8984375
Outputs:
- layer_out: bfloat16 [6144, 2048], P('fs', 'tp')
The draws below stay inside these ranges and needn't reach their ends.
All inputs are finite; a program needn't handle non-finite values.
Results may differ from the reference program's by a relative error of at most 0.015.
Values may be sent and summed in bfloat16 or wider, within the bound.
A program may use at most 64 MiB of HBM per device.

```python
import jax
import jax.numpy as jnp
from jax import lax

D = 2048
F = 3072
SEQ_LEN = 128
TOKENS = 6144
N_TP = 2


def with_spikes(values, own_key, source, target, blocks, factor):
    def block_of(dim):
        return (jnp.arange(values.shape[dim]) // (values.shape[dim] // blocks)).reshape((-1,) + (1,) * (values.ndim - 1 - dim))

    one_side = jax.random.permutation(own_key, blocks)[block_of(target)]
    far = (block_of(target) + blocks // 2) % blocks
    return jnp.where((block_of(source) == one_side) | (block_of(source) == far), factor * values, values)


def shard_levels(key, shape, pieces, smallest, high):
    loudness = 1.0
    for axis_at, shards_of in pieces:
        heights = jax.random.uniform(jax.random.fold_in(jax.random.fold_in(key, 6), axis_at), (shards_of,), jnp.float32, smallest / len(pieces), high / len(pieces))
        loudness = loudness * jnp.repeat(jnp.exp(heights), shape[axis_at] // shards_of).reshape((-1,) + (1,) * (len(shape) - 1 - axis_at))
    return loudness


def noise(stream_key, extent, scale, most, pieces=(), kind=jnp.bfloat16):
    values = jax.random.normal(stream_key, extent, jnp.float32) * scale
    if len(pieces) > 0:
        values = shard_levels(stream_key, extent, pieces, -0.22, 0.18) * values
    return jnp.clip(values, min=-most, max=most).astype(kind)


def heavy_noise(stream_key, extent, deviation, bound, cuts, heavy, kind=jnp.bfloat16):
    drawn = deviation * jax.random.normal(stream_key, extent, jnp.float32)
    if cuts:
        drawn = drawn * shard_levels(stream_key, extent, cuts, -0.22, 0.18)
    return jnp.clip(with_spikes(drawn, jax.random.fold_in(stream_key, 3), *heavy), -bound, bound).astype(kind)


def setup_inputs(seed: int = 0) -> dict:
    streams_of = jax.random.split(jax.random.key(seed), 14)
    return {
        "tokens": noise(streams_of[0], (TOKENS, D), 1.0, 6.0, ((0, 16), (1, 2))),
        "outer_gate": noise(streams_of[1], (D, D), D ** -0.5, 0.125, ((0, 16), (1, 2))),
        "inner_gate": noise(streams_of[2], (D, D), D ** -0.5, 0.125, ((0, 16), (1, 2))),
        "mix_value": noise(streams_of[3], (D, D), D ** -0.5, 0.125, ((0, 16), (1, 2))),
        "mix_taps": noise(streams_of[4], (3, D), 0.577, 3.0, ((1, 2),)),
        "mix_out": heavy_noise(streams_of[5], (D, D), D ** -0.5, 0.1875, ((0, 2), (1, 16)), (0, 1, 16, 2.0)),
        "mix_gain": jnp.clip(1.0 + 0.18 * jax.random.normal(streams_of[6], (D,), jnp.float32), 0.099609375, 1.8984375).astype(jnp.bfloat16),
        "ffn_gate": noise(streams_of[7], (D, F), D ** -0.5, 0.125, ((0, 16), (1, 2))),
        "ffn_value": noise(streams_of[8], (D, F), D ** -0.5, 0.125, ((0, 16), (1, 2))),
        "gate_taps": noise(streams_of[9], (3, F), 0.577, 3.0, ((1, 2),)),
        "value_taps": noise(streams_of[10], (3, F), 0.577, 3.0, ((1, 2),)),
        "ffn_down": heavy_noise(streams_of[11], (F, D), F ** -0.5, 0.15625, ((0, 2), (1, 16)), (0, 1, 16, 2.0)),
        "ffn_gain": jnp.clip(1.0 + 0.18 * jax.random.normal(streams_of[12], (D,), jnp.float32), 0.099609375, 1.8984375).astype(jnp.bfloat16),
    }


residual_scale = 8.0 ** 0.25
norm_epsilon = 1e-05

def stored(values):
    return lax.optimization_barrier(values.astype(jnp.bfloat16)).astype(jnp.float32)

def shift_rows(values, offset):
    position = jnp.arange(values.shape[0]) % SEQ_LEN
    shifted = jnp.concatenate([jnp.zeros((offset, values.shape[1]), values.dtype), values[:-offset]], axis=0)
    return jnp.where((position >= offset)[:, None], shifted, jnp.zeros_like(shifted))

def causal_taps(values, taps):
    weights = taps.astype(jnp.float32)
    return values * weights[2] + shift_rows(values, 1) * weights[1] + shift_rows(values, 2) * weights[0]

def norm_rows(hidden, gain):
    mean = lax.optimization_barrier(jnp.mean(hidden, axis=1, keepdims=True))
    spread = lax.optimization_barrier(jnp.mean(jnp.square(hidden - mean), axis=1, keepdims=True))
    return ((hidden - mean) * lax.rsqrt(spread + norm_epsilon) * gain.astype(jnp.float32)).astype(jnp.bfloat16)

def split_sum(left, right):
    width = left.shape[1] // N_TP
    total = jnp.zeros((left.shape[0], right.shape[1]), jnp.float32)
    for index in range(N_TP):
        term = jnp.dot(left[:, index * width:(index + 1) * width], right[index * width:(index + 1) * width], preferred_element_type=jnp.float32)
        total = total + stored(term)
    return total

def reference(tokens, outer_gate, inner_gate, mix_value, mix_taps, mix_out, mix_gain, ffn_gate, ffn_value, gate_taps, value_taps, ffn_down, ffn_gain):
    outer = stored(jnp.dot(tokens, outer_gate, preferred_element_type=jnp.float32))
    inner = stored(jnp.dot(tokens, inner_gate, preferred_element_type=jnp.float32))
    values = stored(jnp.dot(tokens, mix_value, preferred_element_type=jnp.float32))
    gated = (outer * causal_taps(inner * values, mix_taps)).astype(jnp.bfloat16)
    mixer_branch = split_sum(gated, mix_out)
    first = norm_rows(residual_scale * tokens.astype(jnp.float32) + mixer_branch, mix_gain)
    gate_up = stored(jnp.dot(first, ffn_gate, preferred_element_type=jnp.float32))
    value_up = stored(jnp.dot(first, ffn_value, preferred_element_type=jnp.float32))
    hidden = (jax.nn.silu(causal_taps(gate_up, gate_taps)) * causal_taps(value_up, value_taps)).astype(jnp.bfloat16)
    ffn_branch = split_sum(hidden, ffn_down)
    return norm_rows(residual_scale * first.astype(jnp.float32) + ffn_branch, ffn_gain)
```

```python
import jax
import jax.numpy as jnp
from jax import lax
from jax.sharding import PartitionSpec as P

SEQ_LEN = 128


residual_scale = 8.0**0.25
norm_epsilon = 1e-05


def stored(values):
    return lax.optimization_barrier(values.astype(jnp.bfloat16)).astype(jnp.float32)


def shift_rows(values, offset):
    position = jnp.arange(values.shape[0]) % SEQ_LEN
    shifted = jnp.concatenate(
        [jnp.zeros((offset, values.shape[1]), values.dtype), values[:-offset]], axis=0
    )
    return jnp.where((position >= offset)[:, None], shifted, jnp.zeros_like(shifted))


def causal_taps(values, taps):
    weights = taps.astype(jnp.float32)
    return (
        values * weights[2]
        + shift_rows(values, 1) * weights[1]
        + shift_rows(values, 2) * weights[0]
    )


def fold_rows(whole, pieces):
    return tuple((jnp.dot(whole, piece, preferred_element_type=jnp.float32) for piece in pieces))


def norm_shares(prenorm, gain):
    width = prenorm.shape[1] * lax.axis_size("tp")
    row_sums = jnp.sum(prenorm, axis=1)
    row_squares = jnp.sum(prenorm * prenorm, axis=1)
    total, total_squares = lax.psum((row_sums, row_squares), "tp")
    mean = total / width
    spread = total_squares / width - mean * mean
    scaled = (prenorm - mean[:, None]) * lax.rsqrt(spread[:, None] + norm_epsilon)
    return (scaled * gain.astype(jnp.float32)).astype(jnp.bfloat16)


def plain_body(
    tokens,
    outer_gate,
    inner_gate,
    mix_value,
    mix_taps,
    mix_out,
    mix_gain,
    ffn_gate,
    ffn_value,
    gate_taps,
    value_taps,
    ffn_down,
    ffn_gain,
):
    whole_tokens = lax.all_gather(tokens, "tp", axis=1, tiled=True)
    outer, inner, values = fold_rows(
        whole_tokens,
        (
            lax.all_gather(outer_gate, "fs", axis=0, tiled=True),
            lax.all_gather(inner_gate, "fs", axis=0, tiled=True),
            lax.all_gather(mix_value, "fs", axis=0, tiled=True),
        ),
    )
    outer, inner, values = (stored(outer), stored(inner), stored(values))
    gated = (outer * causal_taps(inner * values, mix_taps)).astype(jnp.bfloat16)
    mixer_terms = jnp.dot(
        gated, lax.all_gather(mix_out, "fs", axis=1, tiled=True), preferred_element_type=jnp.float32
    )
    mixer_branch = lax.psum_scatter(
        mixer_terms.astype(jnp.bfloat16), "tp", scatter_dimension=1, tiled=True
    ).astype(jnp.float32)
    first_own = norm_shares(residual_scale * tokens.astype(jnp.float32) + mixer_branch, mix_gain)
    first_whole = lax.all_gather(first_own, "tp", axis=1, tiled=True)
    gate_up, value_up = fold_rows(
        first_whole,
        (
            lax.all_gather(ffn_gate, "fs", axis=0, tiled=True),
            lax.all_gather(ffn_value, "fs", axis=0, tiled=True),
        ),
    )
    gate_up, value_up = (stored(gate_up), stored(value_up))
    hidden = (
        jax.nn.silu(causal_taps(gate_up, gate_taps)) * causal_taps(value_up, value_taps)
    ).astype(jnp.bfloat16)
    ffn_terms = jnp.dot(
        hidden,
        lax.all_gather(ffn_down, "fs", axis=1, tiled=True),
        preferred_element_type=jnp.float32,
    )
    ffn_branch = lax.psum_scatter(
        ffn_terms.astype(jnp.bfloat16), "tp", scatter_dimension=1, tiled=True
    ).astype(jnp.float32)
    return norm_shares(residual_scale * first_own.astype(jnp.float32) + ffn_branch, ffn_gain)


PLANE = 4
LAYERS = 4


def swap_if(flag, first, second):
    return jnp.where(flag, second, first), jnp.where(flag, first, second)


def ordered(index_bits, pieces):
    pieces = list(pieces)
    for bit, flag in enumerate(index_bits):
        step = 1 << bit
        for at in range(len(pieces)):
            if not at & step:
                pieces[at], pieces[at | step] = swap_if(flag, pieces[at], pieces[at | step])
    return pieces


def folded_body(
    tokens,
    outer_gate,
    inner_gate,
    mix_value,
    mix_taps,
    mix_out,
    mix_gain,
    ffn_gate,
    ffn_value,
    gate_taps,
    value_taps,
    ffn_down,
    ffn_gain,
):
    count = lax.axis_size("fs")
    me = lax.axis_index("fs")
    core = lax.axis_index("tp")
    quarter = me % PLANE
    layer = me // PLANE
    x_bit, y_bit = quarter % 2 == 1, quarter // 2 == 1
    everyone = range(count)
    across = lambda r: [(i, i ^ r) for i in everyone]

    def along_fs(value, r):
        return lax.ppermute(value, "fs", across(r))

    def other_core(value):
        return lax.ppermute(value, "tp", [(0, 1), (1, 0)])

    middle = [(i, i ^ (3 * PLANE)) for i in everyone if i // PLANE in (1, 2)]
    outward = [(i, i ^ PLANE) for i in everyone if i // PLANE in (1, 2)]
    is_middle = (layer == 1) | (layer == 2)

    def collect(shares, cut_dim, join_dim):
        def part(r):
            cuts = []
            for share in shares:
                width = share.shape[cut_dim] // PLANE
                cuts.append(
                    lax.dynamic_slice_in_dim(share, (quarter ^ r) * width, width, cut_dim)
                )
            return jnp.concatenate(cuts, axis=cut_dim)

        pieces = [part(0)] + [along_fs(part(r), r) for r in range(1, PLANE)]
        own = jnp.concatenate(ordered((x_bit, y_bit), pieces), axis=join_dim)
        near = along_fs(own, PLANE)
        pair = jnp.concatenate(swap_if(layer % 2 == 1, own, near), axis=join_dim)
        crossed = lax.ppermute(pair, "fs", middle)
        passed = lax.ppermute(crossed, "fs", outward)
        far = jnp.where(is_middle, crossed, passed)
        return jnp.concatenate(swap_if(layer >= 2, pair, far), axis=join_dim)

    def spread(block):
        half = block.shape[0] // 2
        from_x = along_fs(block, 1)
        from_y = along_fs(block, 2)
        far_top = along_fs(from_y[:half], 1)
        far_bottom = along_fs(from_x[half:], 2)
        return [block, from_x, from_y, jnp.concatenate([far_top, far_bottom], axis=0)]

    def with_other(blocks, axis):
        joined = []
        for block in blocks:
            joined.append(
                jnp.concatenate(swap_if(core == 1, block, other_core(block)), axis=axis)
            )
        return jnp.concatenate(joined, axis=0)

    def narrow(value):
        return value.astype(jnp.bfloat16)

    def wide(value):
        return value.astype(jnp.float32)

    def gathered_sum(terms):
        rows = terms.shape[0] // PLANE
        share = rows // 2
        kept = []
        for r in range(PLANE):
            block = terms[r * rows : (r + 1) * rows]
            mine, theirs = swap_if(core == 1, block[:share], block[share:])
            kept.append(mine + wide(other_core(narrow(theirs))))
        own, for_x, for_y, for_far = kept
        half = share // 2
        passing_y = along_fs(narrow(for_far[:half]), 1)
        passing_x = along_fs(narrow(for_far[half:]), 2)
        x_top = along_fs(narrow(for_x[:half]), 1)
        y_bottom = along_fs(narrow(for_y[half:]), 2)
        x_bottom = along_fs(narrow(for_x[half:] + wide(passing_x)), 1)
        y_top = along_fs(narrow(for_y[:half] + wide(passing_y)), 2)
        from_x = jnp.concatenate([x_top, x_bottom], axis=0)
        from_y = jnp.concatenate([y_top, y_bottom], axis=0)
        return own + wide(from_x) + wide(from_y)

    def norm(prenorm, gain):
        mean = jnp.mean(prenorm, axis=1, keepdims=True)
        spread_of = jnp.mean(jnp.square(prenorm - mean), axis=1, keepdims=True)
        return narrow((prenorm - mean) * lax.rsqrt(spread_of + norm_epsilon) * wide(gain))

    def whole_gain(gain):
        return jnp.concatenate(swap_if(core == 1, gain, other_core(gain)), axis=0)

    def own_quarter(taps):
        width = taps.shape[1] // PLANE
        return lax.dynamic_slice_in_dim(taps, quarter * width, width, 1)

    def dot(left, right):
        return jnp.dot(left, right, preferred_element_type=jnp.float32)

    into_mixer = collect((outer_gate, inner_gate, mix_value), 1, 0)
    whole_tokens = with_other(spread(tokens), 1)
    from_mixer = collect((mix_out,), 0, 1)
    into_ffn = collect((ffn_gate, ffn_value), 1, 0)
    from_ffn = collect((ffn_down,), 0, 1)

    outer, inner, values = jnp.split(wide(narrow(dot(whole_tokens, into_mixer))), 3, axis=1)
    gated = narrow(outer * causal_taps(inner * values, own_quarter(mix_taps)))
    branch = gathered_sum(dot(gated, from_mixer))
    share = branch.shape[0]
    own_tokens = lax.dynamic_slice_in_dim(whole_tokens, core * share, share, 0)
    first = norm(residual_scale * wide(own_tokens) + branch, whole_gain(mix_gain))
    whole_first = with_other(spread(first), 0)
    gate_up, value_up = jnp.split(wide(narrow(dot(whole_first, into_ffn))), 2, axis=1)
    hidden = narrow(
        jax.nn.silu(causal_taps(gate_up, own_quarter(gate_taps)))
        * causal_taps(value_up, own_quarter(value_taps))
    )
    branch = gathered_sum(dot(hidden, from_ffn))
    out = norm(residual_scale * wide(first) + branch, whole_gain(ffn_gain))
    width = out.shape[1] // 2
    mine, theirs = swap_if(core == 1, out[:, :width], out[:, width:])
    return jnp.concatenate(swap_if(core == 1, mine, other_core(theirs)), axis=0)


def solution(mesh):
    folds = mesh.shape["fs"] == PLANE * LAYERS and mesh.shape["tp"] == 2
    body = folded_body if folds else plain_body
    placed = (
        P("fs", "tp"),
        P("fs", "tp"),
        P("fs", "tp"),
        P("fs", "tp"),
        P(None, "tp"),
        P("tp", "fs"),
        P("tp"),
        P("fs", "tp"),
        P("fs", "tp"),
        P(None, "tp"),
        P(None, "tp"),
        P("tp", "fs"),
        P("tp"),
    )
    return jax.shard_map(body, mesh=mesh, in_specs=placed, out_specs=P("fs", "tp"), check_vma=False)
```

```python
import jax
import jax.numpy as jnp
from jax import lax
from jax.sharding import PartitionSpec as P

SEQ_LEN = 128


residual_scale = 8.0**0.25
norm_epsilon = 1e-05


def stored(values):
    return lax.optimization_barrier(values.astype(jnp.bfloat16)).astype(jnp.float32)


def shift_rows(values, offset):
    position = jnp.arange(values.shape[0]) % SEQ_LEN
    shifted = jnp.concatenate(
        [jnp.zeros((offset, values.shape[1]), values.dtype), values[:-offset]], axis=0
    )
    return jnp.where((position >= offset)[:, None], shifted, jnp.zeros_like(shifted))


def causal_taps(values, taps):
    weights = taps.astype(jnp.float32)
    return (
        values * weights[2]
        + shift_rows(values, 1) * weights[1]
        + shift_rows(values, 2) * weights[0]
    )


def fold_rows(whole, pieces):
    return tuple((jnp.dot(whole, piece, preferred_element_type=jnp.float32) for piece in pieces))


def norm_shares(prenorm, gain):
    width = prenorm.shape[1] * lax.axis_size("tp")
    row_sums = jnp.sum(prenorm, axis=1)
    row_squares = jnp.sum(prenorm * prenorm, axis=1)
    total, total_squares = lax.psum((row_sums, row_squares), "tp")
    mean = total / width
    spread = total_squares / width - mean * mean
    scaled = (prenorm - mean[:, None]) * lax.rsqrt(spread[:, None] + norm_epsilon)
    return (scaled * gain.astype(jnp.float32)).astype(jnp.bfloat16)


def plain_body(
    tokens,
    outer_gate,
    inner_gate,
    mix_value,
    mix_taps,
    mix_out,
    mix_gain,
    ffn_gate,
    ffn_value,
    gate_taps,
    value_taps,
    ffn_down,
    ffn_gain,
):
    whole_tokens = lax.all_gather(tokens, "tp", axis=1, tiled=True)
    outer, inner, values = fold_rows(
        whole_tokens,
        (
            lax.all_gather(outer_gate, "fs", axis=0, tiled=True),
            lax.all_gather(inner_gate, "fs", axis=0, tiled=True),
            lax.all_gather(mix_value, "fs", axis=0, tiled=True),
        ),
    )
    outer, inner, values = (stored(outer), stored(inner), stored(values))
    gated = (outer * causal_taps(inner * values, mix_taps)).astype(jnp.bfloat16)
    mixer_terms = jnp.dot(
        gated, lax.all_gather(mix_out, "fs", axis=1, tiled=True), preferred_element_type=jnp.float32
    )
    mixer_branch = lax.psum_scatter(
        mixer_terms.astype(jnp.bfloat16), "tp", scatter_dimension=1, tiled=True
    ).astype(jnp.float32)
    first_own = norm_shares(residual_scale * tokens.astype(jnp.float32) + mixer_branch, mix_gain)
    first_whole = lax.all_gather(first_own, "tp", axis=1, tiled=True)
    gate_up, value_up = fold_rows(
        first_whole,
        (
            lax.all_gather(ffn_gate, "fs", axis=0, tiled=True),
            lax.all_gather(ffn_value, "fs", axis=0, tiled=True),
        ),
    )
    gate_up, value_up = (stored(gate_up), stored(value_up))
    hidden = (
        jax.nn.silu(causal_taps(gate_up, gate_taps)) * causal_taps(value_up, value_taps)
    ).astype(jnp.bfloat16)
    ffn_terms = jnp.dot(
        hidden,
        lax.all_gather(ffn_down, "fs", axis=1, tiled=True),
        preferred_element_type=jnp.float32,
    )
    ffn_branch = lax.psum_scatter(
        ffn_terms.astype(jnp.bfloat16), "tp", scatter_dimension=1, tiled=True
    ).astype(jnp.float32)
    return norm_shares(residual_scale * first_own.astype(jnp.float32) + ffn_branch, ffn_gain)


PLANE = 4
LAYERS = 4


def swap_if(flag, first, second):
    return jnp.where(flag, second, first), jnp.where(flag, first, second)


def ordered(index_bits, pieces):
    pieces = list(pieces)
    for bit, flag in enumerate(index_bits):
        step = 1 << bit
        for at in range(len(pieces)):
            if not at & step:
                pieces[at], pieces[at | step] = swap_if(flag, pieces[at], pieces[at | step])
    return pieces


def folded_body(
    tokens,
    outer_gate,
    inner_gate,
    mix_value,
    mix_taps,
    mix_out,
    mix_gain,
    ffn_gate,
    ffn_value,
    gate_taps,
    value_taps,
    ffn_down,
    ffn_gain,
):
    count = lax.axis_size("fs")
    me = lax.axis_index("fs")
    core = lax.axis_index("tp")
    quarter = me % PLANE
    layer = me // PLANE
    x_bit, y_bit = quarter % 2 == 1, quarter // 2 == 1
    everyone = range(count)
    across = lambda r: [(i, i ^ r) for i in everyone]

    def along_fs(value, r):
        return lax.ppermute(value, "fs", across(r))

    def other_core(value):
        return lax.ppermute(value, "tp", [(0, 1), (1, 0)])

    middle = [(i, i ^ (3 * PLANE)) for i in everyone if i // PLANE in (1, 2)]
    outward = [(i, i ^ PLANE) for i in everyone if i // PLANE in (1, 2)]
    is_middle = (layer == 1) | (layer == 2)

    def exchange(shares, cut_dim, join_dim):
        def part(r):
            cuts = []
            for share in shares:
                width = share.shape[cut_dim] // PLANE
                cuts.append(
                    lax.dynamic_slice_in_dim(share, (quarter ^ r) * width, width, cut_dim)
                )
            return jnp.concatenate(cuts, axis=cut_dim)

        pieces = [part(0)] + [along_fs(part(r), r) for r in range(1, PLANE)]
        return jnp.concatenate(ordered((x_bit, y_bit), pieces), axis=join_dim)

    def pair_up(own, join_dim):
        near = along_fs(own, PLANE)
        return jnp.concatenate(swap_if(layer % 2 == 1, own, near), axis=join_dim)

    def cross(pair):
        return lax.ppermute(pair, "fs", middle)

    def pass_on(crossed):
        return jnp.where(is_middle, crossed, lax.ppermute(crossed, "fs", outward))

    def tie(values, *first):
        return lax.optimization_barrier((values, first))[0]

    def spread(block):
        half = block.shape[0] // 2
        from_x = along_fs(block, 1)
        from_y = along_fs(block, 2)
        far_top = along_fs(from_y[:half], 1)
        far_bottom = along_fs(from_x[half:], 2)
        return [block, from_x, from_y, jnp.concatenate([far_top, far_bottom], axis=0)]

    def with_other(block, axis):
        return jnp.concatenate(swap_if(core == 1, block, other_core(block)), axis=axis)

    def narrow(value):
        return value.astype(jnp.bfloat16)

    def wide(value):
        return value.astype(jnp.float32)

    def gathered_sum(blocks, weight):
        kept = [None] * PLANE
        for r in reversed(range(PLANE)):
            block = dot(blocks[r], weight)
            share = block.shape[0] // 2
            mine, theirs = swap_if(core == 1, block[:share], block[share:])
            kept[r] = mine + wide(other_core(narrow(theirs)))
        own, for_x, for_y, for_far = kept
        half = share // 2
        passing_y = along_fs(narrow(for_far[:half]), 1)
        passing_x = along_fs(narrow(for_far[half:]), 2)
        x_top = along_fs(narrow(for_x[:half]), 1)
        y_bottom = along_fs(narrow(for_y[half:]), 2)
        x_bottom = along_fs(narrow(for_x[half:] + wide(passing_x)), 1)
        y_top = along_fs(narrow(for_y[:half] + wide(passing_y)), 2)
        from_x = jnp.concatenate([x_top, x_bottom], axis=0)
        from_y = jnp.concatenate([y_top, y_bottom], axis=0)
        return own + wide(from_x) + wide(from_y)

    def norm(prenorm, gain):
        mean = jnp.mean(prenorm, axis=1, keepdims=True)
        spread_of = jnp.mean(jnp.square(prenorm - mean), axis=1, keepdims=True)
        return narrow((prenorm - mean) * lax.rsqrt(spread_of + norm_epsilon) * wide(gain))

    def whole_gain(gain):
        return jnp.concatenate(swap_if(core == 1, gain, other_core(gain)), axis=0)

    def own_quarter(taps):
        width = taps.shape[1] // PLANE
        return lax.dynamic_slice_in_dim(taps, quarter * width, width, 1)

    def dot(left, right):
        return jnp.dot(left, right, preferred_element_type=jnp.float32)

    mixer_own = exchange((outer_gate, inner_gate, mix_value), 1, 0)
    mixer_pairs = [pair_up(own, 0) for own in jnp.split(mixer_own, 3, axis=1)]
    tokens_later, out_later = tie((tokens, mix_out), mixer_own)
    mix_out_pair = pair_up(exchange((out_later,), 0, 1), 1)
    token_blocks = spread(tokens_later)
    token_others = [other_core(block) for block in token_blocks]
    gate_later, value_later, down_later = tie(
        (ffn_gate, ffn_value, ffn_down), token_blocks[1], token_blocks[2], mix_out_pair
    )
    ffn_own = exchange((gate_later, value_later), 1, 0)
    down_own = exchange((down_later,), 0, 1)
    mixer_crossed = [cross(pair) for pair in mixer_pairs]
    mix_out_crossed = cross(mix_out_pair)
    ffn_pairs = [pair_up(own, 0) for own in jnp.split(ffn_own, 2, axis=1)]
    down_pair = pair_up(down_own, 1)
    mixer_far = [pass_on(crossed) for crossed in mixer_crossed]
    ffn_crossed = [cross(pair) for pair in ffn_pairs]

    near_first = (layer >= 2) != (core == 1)
    into_mixer = [swap_if(near_first, pair, far) for pair, far in zip(mixer_pairs, mixer_far)]
    into_mixer = tie(into_mixer, *ffn_pairs)
    mixer_taps = own_quarter(mix_taps)
    gated = []
    for block, other in zip(token_blocks, token_others):
        outer, inner, values = (
            wide(narrow(dot(block, mine) + dot(other, theirs))) for mine, theirs in into_mixer
        )
        gated.append(narrow(outer * causal_taps(inner * values, mixer_taps)))
    from_mixer = jnp.concatenate(
        swap_if(layer >= 2, mix_out_pair, pass_on(mix_out_crossed)), axis=1
    )
    branch = gathered_sum(gated, from_mixer)
    share = branch.shape[0]
    rows = core * share
    own_tokens = jnp.concatenate(
        swap_if(
            core == 1,
            lax.dynamic_slice_in_dim(token_blocks[0], rows, share, 0),
            lax.dynamic_slice_in_dim(token_others[0], rows, share, 0),
        ),
        axis=1,
    )
    first = norm(residual_scale * wide(own_tokens) + branch, whole_gain(mix_gain))
    ffn_far = [pass_on(crossed) for crossed in ffn_crossed]
    down_crossed = cross(down_pair)
    first_blocks = [with_other(block, 0) for block in spread(tie(first, *ffn_crossed))]
    into_ffn = [swap_if(layer >= 2, pair, far) for pair, far in zip(ffn_pairs, ffn_far)]
    into_ffn = tie(into_ffn, down_crossed)
    half = first_blocks[0].shape[1] // 2
    own_gate_taps, own_value_taps = own_quarter(gate_taps), own_quarter(value_taps)
    hidden = []
    for block in first_blocks:
        gate_up, value_up = (
            wide(narrow(dot(block[:, :half], low) + dot(block[:, half:], high)))
            for low, high in into_ffn
        )
        hidden.append(
            narrow(
                jax.nn.silu(causal_taps(gate_up, own_gate_taps))
                * causal_taps(value_up, own_value_taps)
            )
        )
    from_ffn = jnp.concatenate(swap_if(layer >= 2, down_pair, pass_on(down_crossed)), axis=1)
    branch = gathered_sum(hidden, from_ffn)
    out = norm(residual_scale * wide(first) + branch, whole_gain(ffn_gain))
    width = out.shape[1] // 2
    mine, theirs = swap_if(core == 1, out[:, :width], out[:, width:])
    return jnp.concatenate(swap_if(core == 1, mine, other_core(theirs)), axis=0)


def solution(mesh):
    folds = mesh.shape["fs"] == PLANE * LAYERS and mesh.shape["tp"] == 2
    body = folded_body if folds else plain_body
    placed = (
        P("fs", "tp"),
        P("fs", "tp"),
        P("fs", "tp"),
        P("fs", "tp"),
        P(None, "tp"),
        P("tp", "fs"),
        P("tp"),
        P("fs", "tp"),
        P("fs", "tp"),
        P(None, "tp"),
        P(None, "tp"),
        P("tp", "fs"),
        P("tp"),
    )
    return jax.shard_map(body, mesh=mesh, in_specs=placed, out_specs=P("fs", "tp"), check_vma=False)
```

```python
import jax
import jax.numpy as jnp
from jax import lax
from jax.sharding import PartitionSpec as P

SEQ_LEN = 128


residual_scale = 8.0**0.25
norm_epsilon = 1e-05


def stored(values):
    return lax.optimization_barrier(values.astype(jnp.bfloat16)).astype(jnp.float32)


def shift_rows(values, offset):
    position = jnp.arange(values.shape[0]) % SEQ_LEN
    shifted = jnp.concatenate(
        [jnp.zeros((offset, values.shape[1]), values.dtype), values[:-offset]], axis=0
    )
    return jnp.where((position >= offset)[:, None], shifted, jnp.zeros_like(shifted))


def causal_taps(values, taps):
    weights = taps.astype(jnp.float32)
    return (
        values * weights[2]
        + shift_rows(values, 1) * weights[1]
        + shift_rows(values, 2) * weights[0]
    )


def fold_rows(whole, pieces):
    return tuple((jnp.dot(whole, piece, preferred_element_type=jnp.float32) for piece in pieces))


def norm_shares(prenorm, gain):
    width = prenorm.shape[1] * lax.axis_size("tp")
    row_sums = jnp.sum(prenorm, axis=1)
    row_squares = jnp.sum(prenorm * prenorm, axis=1)
    total, total_squares = lax.psum((row_sums, row_squares), "tp")
    mean = total / width
    spread = total_squares / width - mean * mean
    scaled = (prenorm - mean[:, None]) * lax.rsqrt(spread[:, None] + norm_epsilon)
    return (scaled * gain.astype(jnp.float32)).astype(jnp.bfloat16)


def plain_body(
    tokens,
    outer_gate,
    inner_gate,
    mix_value,
    mix_taps,
    mix_out,
    mix_gain,
    ffn_gate,
    ffn_value,
    gate_taps,
    value_taps,
    ffn_down,
    ffn_gain,
):
    whole_tokens = lax.all_gather(tokens, "tp", axis=1, tiled=True)
    outer, inner, values = fold_rows(
        whole_tokens,
        (
            lax.all_gather(outer_gate, "fs", axis=0, tiled=True),
            lax.all_gather(inner_gate, "fs", axis=0, tiled=True),
            lax.all_gather(mix_value, "fs", axis=0, tiled=True),
        ),
    )
    outer, inner, values = (stored(outer), stored(inner), stored(values))
    gated = (outer * causal_taps(inner * values, mix_taps)).astype(jnp.bfloat16)
    mixer_terms = jnp.dot(
        gated, lax.all_gather(mix_out, "fs", axis=1, tiled=True), preferred_element_type=jnp.float32
    )
    mixer_branch = lax.psum_scatter(
        mixer_terms.astype(jnp.bfloat16), "tp", scatter_dimension=1, tiled=True
    ).astype(jnp.float32)
    first_own = norm_shares(residual_scale * tokens.astype(jnp.float32) + mixer_branch, mix_gain)
    first_whole = lax.all_gather(first_own, "tp", axis=1, tiled=True)
    gate_up, value_up = fold_rows(
        first_whole,
        (
            lax.all_gather(ffn_gate, "fs", axis=0, tiled=True),
            lax.all_gather(ffn_value, "fs", axis=0, tiled=True),
        ),
    )
    gate_up, value_up = (stored(gate_up), stored(value_up))
    hidden = (
        jax.nn.silu(causal_taps(gate_up, gate_taps)) * causal_taps(value_up, value_taps)
    ).astype(jnp.bfloat16)
    ffn_terms = jnp.dot(
        hidden,
        lax.all_gather(ffn_down, "fs", axis=1, tiled=True),
        preferred_element_type=jnp.float32,
    )
    ffn_branch = lax.psum_scatter(
        ffn_terms.astype(jnp.bfloat16), "tp", scatter_dimension=1, tiled=True
    ).astype(jnp.float32)
    return norm_shares(residual_scale * first_own.astype(jnp.float32) + ffn_branch, ffn_gain)


PLANE = 4
LAYERS = 4


def swap_if(flag, first, second):
    return jnp.where(flag, second, first), jnp.where(flag, first, second)


def ordered(index_bits, pieces):
    pieces = list(pieces)
    for bit, flag in enumerate(index_bits):
        step = 1 << bit
        for at in range(len(pieces)):
            if not at & step:
                pieces[at], pieces[at | step] = swap_if(flag, pieces[at], pieces[at | step])
    return pieces


def folded_body(
    tokens,
    outer_gate,
    inner_gate,
    mix_value,
    mix_taps,
    mix_out,
    mix_gain,
    ffn_gate,
    ffn_value,
    gate_taps,
    value_taps,
    ffn_down,
    ffn_gain,
):
    count = lax.axis_size("fs")
    me = lax.axis_index("fs")
    core = lax.axis_index("tp")
    quarter = me % PLANE
    layer = me // PLANE
    x_bit, y_bit = quarter % 2 == 1, quarter // 2 == 1
    everyone = range(count)
    across = lambda r: [(i, i ^ r) for i in everyone]

    def along_fs(value, r):
        return lax.ppermute(value, "fs", across(r))

    def other_core(value):
        return lax.ppermute(value, "tp", [(0, 1), (1, 0)])

    middle = [(i, i ^ (3 * PLANE)) for i in everyone if i // PLANE in (1, 2)]
    outward = [(i, i ^ PLANE) for i in everyone if i // PLANE in (1, 2)]
    is_middle = (layer == 1) | (layer == 2)

    def exchange(shares, cut_dim, join_dim):
        def part(r):
            cuts = []
            for share in shares:
                width = share.shape[cut_dim] // PLANE
                cuts.append(
                    lax.dynamic_slice_in_dim(share, (quarter ^ r) * width, width, cut_dim)
                )
            return jnp.concatenate(cuts, axis=cut_dim)

        pieces = [part(0)] + [along_fs(part(r), r) for r in range(1, PLANE)]
        return jnp.concatenate(ordered((x_bit, y_bit), pieces), axis=join_dim)

    def pair_up(own, join_dim):
        near = along_fs(own, PLANE)
        return jnp.concatenate(swap_if(layer % 2 == 1, own, near), axis=join_dim)

    def cross(pair):
        return lax.ppermute(pair, "fs", middle)

    def pass_on(crossed):
        return jnp.where(is_middle, crossed, lax.ppermute(crossed, "fs", outward))

    def tie(values, *first):
        return lax.optimization_barrier((values, first))[0]

    def spread(block):
        half = block.shape[0] // 2
        from_x = along_fs(block, 1)
        from_y = along_fs(block, 2)
        far_top = along_fs(from_y[:half], 1)
        far_bottom = along_fs(from_x[half:], 2)
        return [block, from_x, from_y, jnp.concatenate([far_top, far_bottom], axis=0)]

    def with_other(block, axis):
        return jnp.concatenate(swap_if(core == 1, block, other_core(block)), axis=axis)

    def narrow(value):
        return value.astype(jnp.bfloat16)

    def wide(value):
        return value.astype(jnp.float32)

    def gathered_sum(terms):
        rows = terms.shape[0] // PLANE
        share = rows // 2
        kept = [None] * PLANE
        for r in reversed(range(PLANE)):
            block = terms[r * rows : (r + 1) * rows]
            mine, theirs = swap_if(core == 1, block[:share], block[share:])
            kept[r] = mine + wide(other_core(narrow(theirs)))
        own, for_x, for_y, for_far = kept
        half = share // 2
        passing_y = along_fs(narrow(for_far[:half]), 1)
        passing_x = along_fs(narrow(for_far[half:]), 2)
        x_top = along_fs(narrow(for_x[:half]), 1)
        y_bottom = along_fs(narrow(for_y[half:]), 2)
        x_bottom = along_fs(narrow(for_x[half:] + wide(passing_x)), 1)
        y_top = along_fs(narrow(for_y[:half] + wide(passing_y)), 2)
        from_x = jnp.concatenate([x_top, x_bottom], axis=0)
        from_y = jnp.concatenate([y_top, y_bottom], axis=0)
        return own + wide(from_x) + wide(from_y)

    def norm(prenorm, gain):
        mean = jnp.mean(prenorm, axis=1, keepdims=True)
        spread_of = jnp.mean(jnp.square(prenorm - mean), axis=1, keepdims=True)
        return narrow((prenorm - mean) * lax.rsqrt(spread_of + norm_epsilon) * wide(gain))

    def whole_gain(gain):
        return jnp.concatenate(swap_if(core == 1, gain, other_core(gain)), axis=0)

    def own_quarter(taps):
        width = taps.shape[1] // PLANE
        return lax.dynamic_slice_in_dim(taps, quarter * width, width, 1)

    def dot(left, right):
        return jnp.dot(left, right, preferred_element_type=jnp.float32)

    mixer_own = exchange((outer_gate, inner_gate, mix_value), 1, 0)
    mixer_pairs = [pair_up(own, 0) for own in jnp.split(mixer_own, 3, axis=1)]
    tokens_later, out_later = tie((tokens, mix_out), mixer_own)
    mix_out_pair = pair_up(exchange((out_later,), 0, 1), 1)
    token_blocks = spread(tokens_later)
    token_others = [other_core(block) for block in token_blocks]
    gate_later, value_later, down_later = tie(
        (ffn_gate, ffn_value, ffn_down), token_blocks[1], token_blocks[2], mix_out_pair
    )
    ffn_own = exchange((gate_later, value_later), 1, 0)
    down_own = exchange((down_later,), 0, 1)
    mixer_crossed = [cross(pair) for pair in mixer_pairs]
    mix_out_crossed = cross(mix_out_pair)
    mixer_far = [pass_on(crossed) for crossed in mixer_crossed]
    ffn_own = tie(ffn_own, mixer_far[0])
    ffn_pairs = jnp.split(pair_up(ffn_own, 0), 2, axis=1)
    down_pair = pair_up(tie(down_own, *mixer_far), 1)
    ffn_crossed = [cross(pair) for pair in ffn_pairs]

    near_first = (layer >= 2) != (core == 1)
    into_mixer = [swap_if(near_first, pair, far) for pair, far in zip(mixer_pairs, mixer_far)]
    for_mine, for_theirs = (jnp.concatenate(half, axis=1) for half in zip(*into_mixer))
    token_rows = jnp.concatenate(token_blocks, axis=0)
    other_rows = jnp.concatenate(token_others, axis=0)
    projected = narrow(dot(token_rows, for_mine) + dot(other_rows, for_theirs))
    outer, inner, values = jnp.split(wide(projected), 3, axis=1)
    gated = narrow(outer * causal_taps(inner * values, own_quarter(mix_taps)))
    gated = tie(gated, *ffn_pairs)
    from_mixer = jnp.concatenate(
        swap_if(layer >= 2, mix_out_pair, pass_on(mix_out_crossed)), axis=1
    )
    branch = gathered_sum(dot(gated, from_mixer))
    share = branch.shape[0]
    rows = core * share
    own_tokens = jnp.concatenate(
        swap_if(
            core == 1,
            lax.dynamic_slice_in_dim(token_blocks[0], rows, share, 0),
            lax.dynamic_slice_in_dim(token_others[0], rows, share, 0),
        ),
        axis=1,
    )
    first = norm(residual_scale * wide(own_tokens) + branch, whole_gain(mix_gain))
    ffn_far = [pass_on(crossed) for crossed in ffn_crossed]
    down_crossed = cross(down_pair)
    first_blocks = [with_other(block, 0) for block in spread(tie(first, *ffn_crossed))]
    into_ffn = [swap_if(layer >= 2, pair, far) for pair, far in zip(ffn_pairs, ffn_far)]
    into_ffn = tie(into_ffn, down_crossed)
    gate_weight, value_weight = (jnp.concatenate(halves, axis=0) for halves in into_ffn)
    whole_first = jnp.concatenate(first_blocks, axis=0)
    gate_up = wide(narrow(dot(whole_first, gate_weight)))
    value_up = wide(narrow(dot(whole_first, value_weight)))
    hidden = narrow(
        jax.nn.silu(causal_taps(gate_up, own_quarter(gate_taps)))
        * causal_taps(value_up, own_quarter(value_taps))
    )
    from_ffn = jnp.concatenate(swap_if(layer >= 2, down_pair, pass_on(down_crossed)), axis=1)
    branch = gathered_sum(dot(hidden, from_ffn))
    out = norm(residual_scale * wide(first) + branch, whole_gain(ffn_gain))
    width = out.shape[1] // 2
    mine, theirs = swap_if(core == 1, out[:, :width], out[:, width:])
    return jnp.concatenate(swap_if(core == 1, mine, other_core(theirs)), axis=0)


def solution(mesh):
    folds = mesh.shape["fs"] == PLANE * LAYERS and mesh.shape["tp"] == 2
    body = folded_body if folds else plain_body
    placed = (
        P("fs", "tp"),
        P("fs", "tp"),
        P("fs", "tp"),
        P("fs", "tp"),
        P(None, "tp"),
        P("tp", "fs"),
        P("tp"),
        P("fs", "tp"),
        P("fs", "tp"),
        P(None, "tp"),
        P(None, "tp"),
        P("tp", "fs"),
        P("tp"),
    )
    return jax.shard_map(body, mesh=mesh, in_specs=placed, out_specs=P("fs", "tp"), check_vma=False)
```
